512 devices in a mesh: sp: 64 (over z, y), tp: 8 (over x, core).
Axes of the slice: x: 4, y: 8, z: 8, core: 2. Of those that a mesh axis runs over, the one named last changes fastest.
Arguments:
- queries: bfloat16 [32768, 2048], P('sp', 'tp'), may hold values from -14 to 14
- key_states: bfloat16 [32768, 512], P('sp', 'tp'), may hold values from -14 to 14
- value_states: bfloat16 [32768, 512], P('sp', 'tp'), may hold values from -6 to 6
- sink_logits: float32 [32], P('tp'), may hold values from 0 to 5
- out_weight: bfloat16 [2048, 2048], P('tp'), may hold values from -0.125 to 0.125
- residual: bfloat16 [32768, 2048], P(('sp', 'tp')), may hold values from -6 to 6
- gain_attn: float32 [2048], replicated, may hold values from 0.1 to 1.9
- gain_before: float32 [2048], replicated, may hold values from 0.1 to 1.9
- gain_after: float32 [2048], replicated, may hold values from 0.1 to 1.9
- gate_weight: bfloat16 [2048, 5632], P('sp', 'tp'), may hold values from -0.125 to 0.125
- value_weight: bfloat16 [2048, 5632], P('sp', 'tp'), may hold values from -0.125 to 0.125
- gate_taps: float32 [3, 5632], P(None, 'tp'), may hold values from -3 to 3
- value_taps: float32 [3, 5632], P(None, 'tp'), may hold values from -3 to 3
- down_weight: bfloat16 [5632, 2048], P('tp', 'sp'), may hold values from -0.078125 to 0.078125
Outputs:
- layer_out: bfloat16 [32768, 2048], P(('sp', 'tp'))
The draws below stay inside these ranges and needn't reach their ends.
All inputs are finite; a program needn't handle non-finite values.
Results may differ from the reference program's by a relative error of at most 0.018.
Values may be sent and summed in bfloat16 or wider, within the bound.
No kernel may reach another device: no remote copies, remote signals or barrier semaphores. Data moves between devices by JAX's collectives and lax.ppermute only.
A program may use at most 64 MiB of HBM per device.

```python
import jax
import jax.numpy as jnp
from jax import lax

D = 2048
HQ = 32
KV = 8
HD = 64
FF = 5632
WINDOW = 128
CONVK = 3
TOKENS = 32768
N_TP = 8


def drawn_keys(key):
    base = jax.random.truncated_normal(jax.random.fold_in(key, 11), -2.5, 2.5, (TOKENS, KV * HD), jnp.float32)
    return base


def draw_key_states(key, part):
    base = drawn_keys(key)
    return base.astype(jnp.bfloat16)


def draw_queries(key, part):
    own = jax.random.truncated_normal(jax.random.fold_in(key, 21), -2.5, 2.5, (TOKENS, HQ * HD), jnp.float32)
    return own.astype(jnp.bfloat16)


def block_scale(key, shape, cuts, smallest, high):
    loudness, own = 1.0, jax.random.fold_in(key, 6)
    for axis_at, blocks in cuts:
        steps = jnp.exp(jax.random.uniform(jax.random.fold_in(own, axis_at), (blocks,), jnp.float32, smallest / len(cuts), high / len(cuts)))
        loudness = loudness * jnp.repeat(steps, shape[axis_at] // blocks).reshape([-1 if axis == axis_at else 1 for axis in range(len(shape))])
    return loudness


def scatter_about(rng, extent, scale, most, shards=(), kind=jnp.bfloat16):
    loudness = block_scale(rng, extent, shards, -0.22, 0.18) if shards else 1.0
    drawn = jax.random.normal(rng, extent, jnp.float32) * scale * loudness
    return jnp.minimum(jnp.maximum(drawn, -most), most).astype(kind)


def setup_inputs(seed: int = 0) -> dict:
    arg_keys = jax.random.split(jax.random.key(seed), 15)
    return {
        "queries": draw_queries(jax.random.fold_in(arg_keys[14], 71), 0),
        "key_states": draw_key_states(jax.random.fold_in(arg_keys[14], 71), 0),
        "value_states": scatter_about(arg_keys[2], (TOKENS, KV * HD), 1.0, 6.0, ((0, 64), (1, 8))),
        "sink_logits": jnp.clip(5.0 * jax.random.uniform(arg_keys[3], (HQ,), jnp.float32) ** block_scale(arg_keys[3], (HQ,), ((0, 8),), -0.2, 0.2), 0.0, 5.0),
        "out_weight": scatter_about(arg_keys[4], (HQ * HD, D), (HQ * HD) ** -0.5, 0.125, ((0, 8),)),
        "residual": scatter_about(arg_keys[5], (TOKENS, D), 1.0, 6.0, ((0, 512),)),
        "gain_attn": jnp.clip(1.0 + 0.18 * jax.random.normal(arg_keys[6], (D,), jnp.float32), 0.1, 1.9),
        "gain_before": jnp.clip(1.0 + 0.18 * jax.random.normal(arg_keys[7], (D,), jnp.float32), 0.1, 1.9),
        "gain_after": jnp.clip(1.0 + 0.18 * jax.random.normal(arg_keys[8], (D,), jnp.float32), 0.1, 1.9),
        "gate_weight": scatter_about(arg_keys[9], (D, FF), D ** -0.5, 0.125, ((0, 64), (1, 8))),
        "value_weight": scatter_about(arg_keys[10], (D, FF), D ** -0.5, 0.125, ((0, 64), (1, 8))),
        "gate_taps": scatter_about(arg_keys[11], (CONVK, FF), 0.577, 3.0, ((1, 8),), jnp.float32),
        "value_taps": scatter_about(arg_keys[12], (CONVK, FF), 0.577, 3.0, ((1, 8),), jnp.float32),
        "down_weight": scatter_about(arg_keys[13], (FF, D), FF ** -0.5, 0.078125, ((0, 8), (1, 64))),
    }


NEG_FILL = -1e+30

def rms_scale(matrix):
    return matrix * lax.rsqrt(lax.optimization_barrier(jnp.mean(matrix * matrix, axis=-1, keepdims=True)) + 1e-06)

def attention(queries, key_states, value_states, sink_logits):
    length = queries.shape[0]
    blocks = length // WINDOW
    grouping = HQ // KV
    zeros_rows = jnp.zeros((WINDOW, KV * HD), jnp.bfloat16)
    keys_ext = jnp.concatenate([zeros_rows, key_states], axis=0).reshape(blocks + 1, WINDOW, KV, HD)
    values_ext = jnp.concatenate([zeros_rows, value_states], axis=0).reshape(blocks + 1, WINDOW, KV, HD)
    key_blocks = jnp.concatenate([keys_ext[:-1], keys_ext[1:]], axis=1)
    value_blocks = jnp.concatenate([values_ext[:-1], values_ext[1:]], axis=1)
    query_blocks = queries.reshape(blocks, WINDOW, KV, grouping, HD)
    qpos = jnp.arange(length, dtype=jnp.int32).reshape(blocks, WINDOW)
    kpos = jnp.concatenate([qpos - WINDOW, qpos], axis=1)
    visible = (kpos[:, None, :] <= qpos[:, :, None]) & (qpos[:, :, None] - kpos[:, None, :] < WINDOW) & (kpos[:, None, :] >= 0)
    sinks_all = sink_logits.reshape(KV, grouping)

    def one_head(inputs):
        query_part, key_part, value_part, sink_part = inputs
        scores = jnp.einsum('nqgd,nkd->ngqk', query_part.astype(jnp.float32), key_part.astype(jnp.float32)) * HD ** (-0.5)
        scores = jnp.where(visible[:, None], scores, NEG_FILL)
        sink_col = sink_part[None, :, None]
        top = jnp.maximum(lax.optimization_barrier(jnp.max(scores, axis=-1)), sink_col)
        expo = jnp.exp(scores - top[..., None])
        total = lax.optimization_barrier(jnp.sum(expo, axis=-1)) + jnp.exp(sink_col - top)
        probs = (expo / total[..., None]).astype(jnp.bfloat16)
        result = jnp.einsum('ngqk,nkd->nqgd', probs.astype(jnp.float32), value_part.astype(jnp.float32))
        return result.astype(jnp.bfloat16)
    heads_out = lax.map(one_head, (jnp.moveaxis(query_blocks, 2, 0), jnp.moveaxis(key_blocks, 2, 0), jnp.moveaxis(value_blocks, 2, 0), sinks_all))
    return jnp.moveaxis(heads_out, 0, 2).reshape(length, HQ * HD)

def grouped_sum(left, right):
    width = left.shape[1] // N_TP
    total = jnp.zeros((left.shape[0], right.shape[1]), jnp.float32)
    for group_index in range(N_TP):
        part = jnp.dot(left[:, group_index * width:(group_index + 1) * width], right[group_index * width:(group_index + 1) * width], preferred_element_type=jnp.float32)
        total = total + part.astype(jnp.bfloat16).astype(jnp.float32)
    return total

def causal_taps(upward, kernel):
    length = upward.shape[0]
    padded = jnp.concatenate([jnp.zeros((CONVK - 1, upward.shape[1]), jnp.bfloat16), upward], axis=0).astype(jnp.float32)
    result = jnp.zeros((length, upward.shape[1]), jnp.float32)
    for tap_index in range(CONVK):
        result = result + kernel[tap_index][None, :] * padded[tap_index:tap_index + length]
    return result

def reference(queries, key_states, value_states, sink_logits, out_weight, residual, gain_attn, gain_before, gain_after, gate_weight, value_weight, gate_taps, value_taps, down_weight):
    attended = attention(queries, key_states, value_states, sink_logits)
    attn_proj = grouped_sum(attended, out_weight)
    middle = residual.astype(jnp.float32) + rms_scale(attn_proj) * gain_attn
    normed = (rms_scale(middle) * gain_before).astype(jnp.bfloat16)
    gate_up = jnp.dot(normed, gate_weight, preferred_element_type=jnp.float32).astype(jnp.bfloat16)
    value_up = jnp.dot(normed, value_weight, preferred_element_type=jnp.float32).astype(jnp.bfloat16)
    gate_conv = causal_taps(gate_up, gate_taps)
    value_conv = causal_taps(value_up, value_taps)
    hidden = (jax.nn.silu(gate_conv) * value_conv).astype(jnp.bfloat16)
    down = grouped_sum(hidden, down_weight)
    return (middle + rms_scale(down) * gain_after).astype(jnp.bfloat16)
```

```python
import functools

import jax
import jax.numpy as jnp
from jax import lax
from jax.experimental import pallas as pl
from jax.experimental.pallas import tpu as pltpu
from jax.sharding import Mesh
from jax.sharding import PartitionSpec as P

HD = 64
WINDOW = 128
D = 2048
UNITS = 704
PADDED = 768
UP_AT = PADDED
WIDE = PADDED + 2 * UNITS
HALO = 16
LOCAL = 512
OWN = 64
SP = ("z", "y")
TP = ("x", "c")

NEG_FILL = -1e30
BLOCKS = tuple((at, min(256, WIDE - at)) for at in range(UP_AT, WIDE, 256))


def passed_along(block, axis, distance):
    devices = range(lax.axis_size(axis))
    route = [(i - distance, i) for i in devices if i - distance in devices]
    return lax.ppermute(block, axis, route)


def in_blocks(shard, dim, peers):
    before, after = (shard.shape[:dim], shard.shape[dim + 1 :])
    return jnp.moveaxis(shard.reshape(*before, peers, -1, *after), dim, 0)


def sum_at_owner(shard, axis, dim):
    peers = lax.axis_size(axis)
    pieces = lax.all_to_all(in_blocks(shard, dim, peers), axis, 0, 0, tiled=True)
    return jnp.sum(pieces.astype(jnp.float32), axis=0)


def sent_to_all(shard, axis):
    copies = jnp.broadcast_to(shard, (lax.axis_size(axis), *shard.shape))
    return lax.all_to_all(copies, axis, split_axis=0, concat_axis=0, tiled=True)


def rms_scale(matrix):
    return matrix * lax.rsqrt(jnp.mean(matrix * matrix, axis=-1, keepdims=True) + 1e-06)


def attention_local(queries, key_states, value_states, sink_logits):
    length = queries.shape[0]
    blocks = length // WINDOW
    kv_local = key_states.shape[1] // HD
    grouping = queries.shape[1] // key_states.shape[1]
    earlier_keys, earlier_values = passed_along(
        (key_states[length - WINDOW :], value_states[length - WINDOW :]), SP, 1
    )
    keys_ext = jnp.concatenate([earlier_keys, key_states], axis=0).reshape(
        blocks + 1, WINDOW, kv_local, HD
    )
    values_ext = jnp.concatenate([earlier_values, value_states], axis=0).reshape(
        blocks + 1, WINDOW, kv_local, HD
    )
    key_blocks = jnp.concatenate([keys_ext[:-1], keys_ext[1:]], axis=1)
    value_blocks = jnp.concatenate([values_ext[:-1], values_ext[1:]], axis=1)
    query_blocks = queries.reshape(blocks, WINDOW, kv_local, grouping, HD)
    offset = lax.axis_index(SP) * length
    qpos = (offset + jnp.arange(length, dtype=jnp.int32)).reshape(blocks, WINDOW)
    kpos = jnp.concatenate([qpos - WINDOW, qpos], axis=1)
    visible = (
        (kpos[:, None, :] <= qpos[:, :, None])
        & (qpos[:, :, None] - kpos[:, None, :] < WINDOW)
        & (kpos[:, None, :] >= 0)
    )
    scores = jnp.einsum(
        "nqhgd,nkhd->nhgqk", query_blocks, key_blocks, preferred_element_type=jnp.float32
    ) * HD ** (-0.5)
    scores = jnp.where(visible[:, None, None], scores, NEG_FILL)
    sink_col = sink_logits.reshape(kv_local, grouping)[None, :, :, None]
    top = jnp.maximum(jnp.max(scores, axis=-1), sink_col)
    expo = jnp.exp(scores - top[..., None])
    total = jnp.sum(expo, axis=-1) + jnp.exp(sink_col - top)
    probs = (expo / total[..., None]).astype(jnp.bfloat16)
    result = jnp.einsum(
        "nhgqk,nkhd->nqhgd", probs, value_blocks, preferred_element_type=jnp.float32
    )
    return result.astype(jnp.bfloat16).reshape(length, queries.shape[1])


def feed_forward_kernel(x_ref, taps_ref, w_hbm, out_ref, w_up, w_down, up, hidden, sems):
    copies = []
    for k, (at, width) in enumerate(BLOCKS):
        copies.append(
            pltpu.make_async_copy(
                w_hbm.at[:, pl.ds(at, width)],
                w_up.at[:, pl.ds(at - UP_AT, width)],
                sems.at[k],
            )
        )
    down_copy = pltpu.make_async_copy(w_hbm.at[:, pl.ds(0, PADDED)], w_down, sems.at[len(BLOCKS)])
    for copy in copies:
        copy.start()
    down_copy.start()
    for (at, width), copy in zip(BLOCKS, copies):
        copy.wait()
        cols = pl.ds(at - UP_AT, width)
        part = jnp.dot(x_ref[...], w_up[:, cols], preferred_element_type=jnp.float32)
        up[:, cols] = part.astype(jnp.bfloat16).astype(jnp.float32)
    rows = 64
    lane = lax.broadcasted_iota(jnp.int32, (rows, PADDED), 1)

    def conv(start, first):
        cols = pl.ds(first, PADDED)
        total = taps_ref[0:1, cols] * up[pl.ds(start + HALO - 2, rows), cols]
        total = total + taps_ref[1:2, cols] * up[pl.ds(start + HALO - 1, rows), cols]
        return total + taps_ref[2:3, cols] * up[pl.ds(start + HALO, rows), cols]

    for start in range(0, LOCAL, rows):
        gate = conv(start, 0)
        value = pltpu.roll(conv(start, 2 * UNITS - PADDED), UNITS, 1)
        both = gate / (1.0 + jnp.exp(-gate)) * value
        both = jnp.where(lane < UNITS, both, 0.0)
        hidden[pl.ds(start, rows), :] = both.astype(jnp.bfloat16)
    down_copy.wait()
    width = 512
    for at in range(0, D, width):
        part = lax.dot_general(
            hidden[...],
            w_down[pl.ds(at, width), :],
            (((1,), (1,)), ((), ())),
            preferred_element_type=jnp.float32,
        ).astype(jnp.bfloat16)
        for block in range(LOCAL // OWN):
            out_ref[block % 2, block // 2, :, pl.ds(at, width)] = part[
                block * OWN : (block + 1) * OWN
            ]


def feed_forward(rows, taps, weights):
    return pl.pallas_call(
        feed_forward_kernel,
        out_shape=jax.ShapeDtypeStruct((2, LOCAL // OWN // 2, OWN, D), jnp.bfloat16),
        in_specs=[
            pl.BlockSpec(memory_space=pltpu.VMEM),
            pl.BlockSpec(memory_space=pltpu.VMEM),
            pl.BlockSpec(memory_space=pltpu.HBM),
        ],
        out_specs=pl.BlockSpec(memory_space=pltpu.VMEM),
        scratch_shapes=[
            pltpu.VMEM((D, 2 * UNITS), jnp.bfloat16),
            pltpu.VMEM((D, PADDED), jnp.bfloat16),
            pltpu.VMEM((HALO + LOCAL, 2 * UNITS), jnp.float32),
            pltpu.VMEM((LOCAL, PADDED), jnp.bfloat16),
            pltpu.SemaphoreType.DMA((len(BLOCKS) + 1,)),
        ],
        compiler_params=pltpu.CompilerParams(vmem_limit_bytes=40 * 1024 * 1024),
        cost_estimate=pl.CostEstimate(
            flops=6 * LOCAL * D * UNITS,
            bytes_accessed=2 * D * WIDE + 4 * LOCAL * D,
            transcendentals=LOCAL * UNITS,
        ),
        name="feed_forward",
    )(rows, taps, weights)


def on_device(
    queries,
    key_states,
    value_states,
    sink_logits,
    out_weight,
    residual,
    gain_attn,
    gain_before,
    gain_after,
    gate_weight,
    value_weight,
    gate_taps,
    value_taps,
    down_weight,
):
    packed = jnp.concatenate(
        [
            jnp.pad(down_weight.T, ((0, 0), (0, PADDED - UNITS))),
            gate_weight,
            value_weight,
        ],
        axis=1,
    )
    weights = lax.all_gather(packed, SP, axis=0, tiled=True)
    taps = jnp.concatenate([gate_taps, value_taps], axis=1)
    attended = attention_local(queries, key_states, value_states, sink_logits)
    attn_proj = sum_at_owner(
        jnp.dot(attended, out_weight, preferred_element_type=jnp.float32).astype(jnp.bfloat16),
        TP,
        0,
    )
    middle = residual.astype(jnp.float32) + rms_scale(attn_proj) * gain_attn
    normed = (rms_scale(middle) * gain_before).astype(jnp.bfloat16)
    whole_rows = sent_to_all(normed, TP).reshape(LOCAL, D)
    earlier = passed_along(whole_rows[LOCAL - HALO :], SP, 1)
    rows = jnp.concatenate([earlier, whole_rows], axis=0)
    shares = feed_forward(rows, taps, weights)
    pair = jnp.sum(
        lax.all_to_all(shares, "c", 0, 0, tiled=True).astype(jnp.float32), axis=0
    ).astype(jnp.bfloat16)
    down = jnp.sum(
        lax.all_to_all(pair, "x", 0, 0, tiled=True).astype(jnp.float32), axis=0
    )
    return (middle + rms_scale(down) * gain_after).astype(jnp.bfloat16)


def solution(mesh):
    mesh = Mesh(mesh.devices.reshape(8, 8, 4, 2), ("z", "y", "x", "c"))
    in_specs = (
        P(SP, TP),
        P(SP, TP),
        P(SP, TP),
        P(TP),
        P(TP, None),
        P((*SP, *TP), None),
        P(),
        P(),
        P(),
        P(SP, TP),
        P(SP, TP),
        P(None, TP),
        P(None, TP),
        P(TP, SP),
    )
    out_specs = P((*SP, *TP), None)
    return jax.shard_map(
        on_device, mesh=mesh, in_specs=in_specs, out_specs=out_specs, check_vma=False
    )
```

```python
import functools

import jax
import jax.numpy as jnp
from jax import lax
from jax.experimental import pallas as pl
from jax.experimental.pallas import tpu as pltpu
from jax.sharding import Mesh
from jax.sharding import PartitionSpec as P

HD = 64
WINDOW = 128
D = 2048
UNITS = 704
PADDED = 768
UP_AT = PADDED
WIDE = PADDED + 2 * UNITS
HALO = 16
LOCAL = 512
OWN = 64
SP = ("z", "y")
TP = ("x", "c")

NEG_FILL = -1e30
ALL = (*SP, *TP)
RING = 8
STEPS = (0, 1, -1, 2, -2, 3, -3, 4)
CHUNKS = ((UP_AT, 512), (UP_AT + 512, 512), (UP_AT + 1024, 384), (0, PADDED))
VMEM_LIMIT = 44 * 1024 * 1024


def passed_along(block, axis, distance):
    devices = range(lax.axis_size(axis))
    route = [(i - distance, i) for i in devices if i - distance in devices]
    return lax.ppermute(block, axis, route)


def summed_at_owner(shares):
    pair = jnp.sum(
        lax.all_to_all(shares, "c", 0, 0, tiled=True).astype(jnp.float32), axis=0
    ).astype(jnp.bfloat16)
    return jnp.sum(lax.all_to_all(pair, "x", 0, 0, tiled=True).astype(jnp.float32), axis=0)


def sent_to_all(shard, axis):
    copies = jnp.broadcast_to(shard, (lax.axis_size(axis), *shard.shape))
    return lax.all_to_all(copies, axis, split_axis=0, concat_axis=0, tiled=True)


def rms_scale(matrix):
    return matrix * lax.rsqrt(jnp.mean(matrix * matrix, axis=-1, keepdims=True) + 1e-06)


def attention_local(queries, key_states, value_states, sink_logits):
    length = queries.shape[0]
    blocks = length // WINDOW
    kv_local = key_states.shape[1] // HD
    grouping = queries.shape[1] // key_states.shape[1]
    earlier_keys, earlier_values = passed_along(
        (key_states[length - WINDOW :], value_states[length - WINDOW :]), SP, 1
    )
    keys_ext = jnp.concatenate([earlier_keys, key_states], axis=0).reshape(
        blocks + 1, WINDOW, kv_local, HD
    )
    values_ext = jnp.concatenate([earlier_values, value_states], axis=0).reshape(
        blocks + 1, WINDOW, kv_local, HD
    )
    key_blocks = jnp.concatenate([keys_ext[:-1], keys_ext[1:]], axis=1)
    value_blocks = jnp.concatenate([values_ext[:-1], values_ext[1:]], axis=1)
    query_blocks = queries.reshape(blocks, WINDOW, kv_local, grouping, HD)
    offset = lax.axis_index(SP) * length
    qpos = (offset + jnp.arange(length, dtype=jnp.int32)).reshape(blocks, WINDOW)
    kpos = jnp.concatenate([qpos - WINDOW, qpos], axis=1)
    visible = (
        (kpos[:, None, :] <= qpos[:, :, None])
        & (qpos[:, :, None] - kpos[:, None, :] < WINDOW)
        & (kpos[:, None, :] >= 0)
    )
    scores = jnp.einsum(
        "nqhgd,nkhd->nhgqk", query_blocks, key_blocks, preferred_element_type=jnp.float32
    ) * HD ** (-0.5)
    scores = jnp.where(visible[:, None, None], scores, NEG_FILL)
    sink_col = sink_logits.reshape(kv_local, grouping)[None, :, :, None]
    top = jnp.maximum(jnp.max(scores, axis=-1), sink_col)
    expo = jnp.exp(scores - top[..., None])
    total = jnp.sum(expo, axis=-1) + jnp.exp(sink_col - top)
    probs = (expo / total[..., None]).astype(jnp.bfloat16)
    result = jnp.einsum(
        "nhgqk,nkhd->nqhgd", probs, value_blocks, preferred_element_type=jnp.float32
    )
    return result.astype(jnp.bfloat16).reshape(length, queries.shape[1])


def feed_forward_kernel(x_ref, taps_ref, *refs):
    blocks = refs[:RING]
    out_ref, weights, up, hidden, sems = refs[RING:]
    core = lax.axis_index("c")
    place = jnp.where(core == 1, lax.axis_index("z"), lax.axis_index("y"))

    def on_copies(chunk, act):
        cols = pl.ds(*CHUNKS[chunk])
        for k, (block, step) in enumerate(zip(blocks, STEPS)):
            source = lax.rem(place - step + RING, RING)
            sem = sems.at[chunk, k]

            @pl.when(core == 1)
            def _():
                act(
                    pltpu.make_async_copy(
                        block.at[:, :, cols], weights.at[source, :, :, cols], sem
                    )
                )

            @pl.when(core == 0)
            def _():
                act(
                    pltpu.make_async_copy(
                        block.at[:, :, cols], weights.at[:, source, :, cols], sem
                    )
                )

    for chunk in range(len(CHUNKS)):
        on_copies(chunk, lambda copy: copy.start())
    for chunk, (at, width) in enumerate(CHUNKS[:-1]):
        on_copies(chunk, lambda copy: copy.wait())
        for sub in range(at, at + width, 256):
            wide = min(256, at + width - sub)
            part = jnp.dot(
                x_ref[...],
                weights[:, :, :, sub : sub + wide].reshape(D, wide),
                preferred_element_type=jnp.float32,
            )
            up[:, sub - UP_AT : sub - UP_AT + wide] = part.astype(jnp.bfloat16).astype(
                jnp.float32
            )
    rows = 64
    lane = lax.broadcasted_iota(jnp.int32, (rows, PADDED), 1)

    def conv(start, first):
        cols = pl.ds(first, PADDED)
        total = taps_ref[0:1, cols] * up[pl.ds(start + HALO - 2, rows), cols]
        total = total + taps_ref[1:2, cols] * up[pl.ds(start + HALO - 1, rows), cols]
        return total + taps_ref[2:3, cols] * up[pl.ds(start + HALO, rows), cols]

    for start in range(0, LOCAL, rows):
        gate = conv(start, 0)
        value = pltpu.roll(conv(start, 2 * UNITS - PADDED), UNITS, 1)
        both = gate / (1.0 + jnp.exp(-gate)) * value
        both = jnp.where(lane < UNITS, both, 0.0)
        hidden[pl.ds(start, rows), :] = both.astype(jnp.bfloat16)
    on_copies(len(CHUNKS) - 1, lambda copy: copy.wait())
    for z in range(0, RING, 2):
        part = lax.dot_general(
            hidden[...],
            weights[z : z + 2, :, :, 0:PADDED].reshape(2 * D // RING, PADDED),
            (((1,), (1,)), ((), ())),
            preferred_element_type=jnp.float32,
        ).astype(jnp.bfloat16)
        cols = pl.ds(z * (D // RING), 2 * D // RING)
        for block in range(LOCAL // OWN):
            out_ref[block % 2, block // 2, :, cols] = part[block * OWN : (block + 1) * OWN]


def feed_forward(rows, taps, blocks):
    return pl.pallas_call(
        feed_forward_kernel,
        out_shape=jax.ShapeDtypeStruct((2, LOCAL // OWN // 2, OWN, D), jnp.bfloat16),
        in_specs=[
            pl.BlockSpec(memory_space=pltpu.VMEM),
            pl.BlockSpec(memory_space=pltpu.VMEM),
        ]
        + [pl.BlockSpec(memory_space=pl.ANY)] * RING,
        out_specs=pl.BlockSpec(memory_space=pltpu.VMEM),
        scratch_shapes=[
            pltpu.VMEM((RING, RING, D // RING // RING, WIDE), jnp.bfloat16),
            pltpu.VMEM((HALO + LOCAL, 2 * UNITS), jnp.float32),
            pltpu.VMEM((LOCAL, PADDED), jnp.bfloat16),
            pltpu.SemaphoreType.DMA((len(CHUNKS), RING)),
        ],
        compiler_params=pltpu.CompilerParams(vmem_limit_bytes=VMEM_LIMIT),
        cost_estimate=pl.CostEstimate(
            flops=6 * LOCAL * D * UNITS,
            bytes_accessed=2 * D * WIDE + 4 * LOCAL * D,
            transcendentals=LOCAL * UNITS,
        ),
        name="feed_forward",
    )(rows, taps, *blocks)


def device_at(z, y, x, c):
    return ((z * RING + y) * 4 + x) * 2 + c


def crossed_groups():
    groups = []
    for x in range(4):
        for fixed in range(RING):
            groups.append([device_at(fixed, k, x, 1) for k in range(RING)])
            groups.append([device_at(k, fixed, x, 0) for k in range(RING)])
    return groups


def ring_step(block, distance):
    route = []
    for z in range(RING):
        for y in range(RING):
            for x in range(4):
                route.append(
                    (device_at(z, y, x, 1), device_at((z + distance) % RING, y, x, 1))
                )
                route.append(
                    (device_at(z, y, x, 0), device_at(z, (y + distance) % RING, x, 0))
                )
    return lax.ppermute(block, ALL, route)


def gathered_blocks(packed):
    copies = jnp.broadcast_to(packed, (RING, *packed.shape))
    own = lax.all_to_all(copies, ALL, 0, 0, tiled=True, axis_index_groups=crossed_groups())
    held = {0: own}
    for step in range(1, RING // 2 + 1):
        held[step] = ring_step(held[step - 1], 1)
        if step < RING // 2:
            held[-step] = ring_step(held[1 - step], -1)
    return [held[step] for step in STEPS]


def on_device(
    queries,
    key_states,
    value_states,
    sink_logits,
    out_weight,
    residual,
    gain_attn,
    gain_before,
    gain_after,
    gate_weight,
    value_weight,
    gate_taps,
    value_taps,
    down_weight,
):
    packed = jnp.concatenate(
        [
            jnp.pad(down_weight.T, ((0, 0), (0, PADDED - UNITS))),
            gate_weight,
            value_weight,
        ],
        axis=1,
    )
    weights = gathered_blocks(packed)
    taps = jnp.concatenate([gate_taps, value_taps], axis=1)
    attended = attention_local(queries, key_states, value_states, sink_logits)
    shares = jnp.dot(attended, out_weight, preferred_element_type=jnp.float32)
    shares = shares.astype(jnp.bfloat16).reshape(LOCAL // OWN // 2, 2, OWN, D)
    attn_proj = summed_at_owner(jnp.moveaxis(shares, 1, 0))
    middle = residual.astype(jnp.float32) + rms_scale(attn_proj) * gain_attn
    normed = (rms_scale(middle) * gain_before).astype(jnp.bfloat16)
    half = sent_to_all(normed, "x")
    whole_rows = jnp.moveaxis(sent_to_all(half, "c"), 0, 1).reshape(LOCAL, D)
    earlier = passed_along(whole_rows[LOCAL - HALO :], SP, 1)
    rows = jnp.concatenate([earlier, whole_rows], axis=0)
    shares = feed_forward(rows, taps, weights)
    down = summed_at_owner(shares)
    return (middle + rms_scale(down) * gain_after).astype(jnp.bfloat16)


def solution(mesh):
    mesh = Mesh(mesh.devices.reshape(8, 8, 4, 2), ("z", "y", "x", "c"))
    in_specs = (
        P(SP, TP),
        P(SP, TP),
        P(SP, TP),
        P(TP),
        P(TP, None),
        P((*SP, *TP), None),
        P(),
        P(),
        P(),
        P(SP, TP),
        P(SP, TP),
        P(None, TP),
        P(None, TP),
        P(TP, SP),
    )
    out_specs = P((*SP, *TP), None)
    return jax.shard_map(
        on_device, mesh=mesh, in_specs=in_specs, out_specs=out_specs, check_vma=False
    )
```

```python
import functools

import jax
import jax.numpy as jnp
from jax import lax
from jax.experimental import pallas as pl
from jax.experimental.pallas import tpu as pltpu
from jax.sharding import Mesh
from jax.sharding import PartitionSpec as P

HD = 64
WINDOW = 128
D = 2048
UNITS = 704
PADDED = 768
UP_AT = PADDED
WIDE = PADDED + 2 * UNITS
HALO = 16
LOCAL = 512
OWN = 64
SP = ("z", "y")
TP = ("x", "c")

NEG_FILL = -1e30
ALL = (*SP, *TP)
RING = 8
STEPS = (0, 1, -1, 2, -2, 3, -3, 4)
CHUNKS = ((UP_AT, 512), (UP_AT + 512, 512), (UP_AT + 1024, 384), (0, PADDED))
VMEM_LIMIT = 44 * 1024 * 1024


def passed_along(block, axis, distance):
    devices = range(lax.axis_size(axis))
    route = [(i - distance, i) for i in devices if i - distance in devices]
    return lax.ppermute(block, axis, route)


def swapped(block):
    return lax.ppermute(block, "c", [(0, 1), (1, 0)])


def projected(rows, weight):
    return jnp.einsum("xrk,kd->xrd", rows, weight, preferred_element_type=jnp.float32)


def summed_over_x(shares):
    return jnp.sum(lax.all_to_all(shares, "x", 0, 0, tiled=True).astype(jnp.float32), axis=0)


def sent_to_all(shard, axis):
    copies = jnp.broadcast_to(shard, (lax.axis_size(axis), *shard.shape))
    return lax.all_to_all(copies, axis, split_axis=0, concat_axis=0, tiled=True)


def rms_scale(matrix):
    return matrix * lax.rsqrt(jnp.mean(matrix * matrix, axis=-1, keepdims=True) + 1e-06)


def attention_kernel(q_ref, k_ref, v_ref, edge_ref, sink_ref, own_ref, other_ref):
    core = lax.axis_index("c")
    first = lax.axis_index("z") + lax.axis_index("y") == 0
    row = lax.broadcasted_iota(jnp.int32, (WINDOW, 2 * WINDOW), 0)
    key = lax.broadcasted_iota(jnp.int32, (WINDOW, 2 * WINDOW), 1)
    inside = (key > row) & (key <= row + WINDOW)
    none = jnp.zeros((HD, 2 * WINDOW), jnp.bfloat16)
    for n in range(LOCAL // WINDOW):
        if n == 0:
            keys = jnp.concatenate([edge_ref[:HD], k_ref[:, :WINDOW]], axis=1)
            values = jnp.concatenate([edge_ref[HD:], v_ref[:, :WINDOW]], axis=1)
            seen = inside & ((key >= WINDOW) | jnp.logical_not(first))
        else:
            cols = pl.ds((n - 1) * WINDOW, 2 * WINDOW)
            keys, values, seen = k_ref[:, cols], v_ref[:, cols], inside
        for pair in range(2):
            cols = pl.ds(pair * 2 * HD, 2 * HD)
            query = q_ref[pl.ds(n * WINDOW, WINDOW), cols]
            result = jnp.zeros((WINDOW, 2 * HD), jnp.float32)
            for odd in range(2):
                placed = lambda part: jnp.concatenate([none, part] if odd else [part, none], axis=0)
                scores = jnp.dot(query, placed(keys), preferred_element_type=jnp.float32)
                scores = jnp.where(seen, scores * HD ** (-0.5), NEG_FILL)
                sink = sink_ref[2 * pair + odd]
                top = jnp.maximum(jnp.max(scores, axis=-1, keepdims=True), sink)
                expo = jnp.exp(scores - top)
                total = jnp.sum(expo, axis=-1, keepdims=True) + jnp.exp(sink - top)
                probs = (expo / total).astype(jnp.bfloat16)
                result = result + lax.dot_general(
                    probs,
                    placed(values),
                    (((1,), (1,)), ((), ())),
                    preferred_element_type=jnp.float32,
                )
            result = result.astype(jnp.bfloat16)

            @pl.when(core == 0)
            def _():
                own_ref[n, :, cols] = result[:OWN]
                other_ref[n, :, cols] = result[OWN:]

            @pl.when(core == 1)
            def _():
                own_ref[n, :, cols] = result[OWN:]
                other_ref[n, :, cols] = result[:OWN]


def attention_local(queries, key_states, value_states, sink_logits):
    keys, values = key_states.T, value_states.T
    edge = jnp.concatenate([keys[:, LOCAL - WINDOW :], values[:, LOCAL - WINDOW :]], axis=0)
    edge = passed_along(edge, SP, 1)
    half = jax.ShapeDtypeStruct((LOCAL // OWN // 2, OWN, 4 * HD), jnp.bfloat16)
    vmem = pl.BlockSpec(memory_space=pltpu.VMEM)
    return pl.pallas_call(
        attention_kernel,
        out_shape=(half, half),
        in_specs=[vmem] * 4 + [pl.BlockSpec(memory_space=pltpu.SMEM)],
        out_specs=(vmem, vmem),
        compiler_params=pltpu.CompilerParams(vmem_limit_bytes=16 * 1024 * 1024),
        cost_estimate=pl.CostEstimate(
            flops=8 * 4 * LOCAL * 2 * WINDOW * HD,
            bytes_accessed=8 * LOCAL * 4 * HD,
            transcendentals=4 * LOCAL * 2 * WINDOW,
        ),
        name="attention",
    )(queries, keys, values, edge, sink_logits)


def feed_forward_kernel(own_ref, other_ref, halo_0, halo_1, taps_ref, *refs):
    blocks = refs[:RING]
    out_own, out_other, weights, x_ref, up, hidden, sems, row_sems = refs[RING:]
    core = lax.axis_index("c")
    place = jnp.where(core == 1, lax.axis_index("z"), lax.axis_index("y"))

    def on_copies(chunk, act):
        cols = pl.ds(*CHUNKS[chunk])
        for k, (block, step) in enumerate(zip(blocks, STEPS)):
            source = lax.rem(place - step + RING, RING)
            sem = sems.at[chunk, k]

            @pl.when(core == 1)
            def _():
                act(
                    pltpu.make_async_copy(
                        block.at[:, :, cols], weights.at[source, :, :, cols], sem
                    )
                )

            @pl.when(core == 0)
            def _():
                act(
                    pltpu.make_async_copy(
                        block.at[:, :, cols], weights.at[:, source, :, cols], sem
                    )
                )

    def on_rows(act):
        for x in range(LOCAL // OWN // 2):
            for k, (part, at) in enumerate(((own_ref, core), (other_ref, 1 - core))):
                start = pl.multiple_of(HALO + OWN * (2 * x + at), HALO)
                act(
                    pltpu.make_async_copy(
                        part.at[x], x_ref.at[pl.ds(start, OWN)], row_sems.at[2 * x + k]
                    )
                )
        for k, halo in enumerate((halo_0, halo_1)):

            @pl.when(core == k)
            def _():
                act(pltpu.make_async_copy(halo, x_ref.at[pl.ds(0, HALO)], row_sems.at[8]))

    on_rows(lambda copy: copy.start())
    for chunk in range(len(CHUNKS)):
        on_copies(chunk, lambda copy: copy.start())
    on_rows(lambda copy: copy.wait())
    for chunk, (at, width) in enumerate(CHUNKS[:-1]):
        on_copies(chunk, lambda copy: copy.wait())
        for sub in range(at, at + width, 256):
            wide = min(256, at + width - sub)
            part = jnp.dot(
                x_ref[...],
                weights[:, :, :, sub : sub + wide].reshape(D, wide),
                preferred_element_type=jnp.float32,
            )
            up[:, sub - UP_AT : sub - UP_AT + wide] = part.astype(jnp.bfloat16).astype(
                jnp.float32
            )
    rows = 64
    lane = lax.broadcasted_iota(jnp.int32, (rows, PADDED), 1)

    def conv(start, first):
        cols = pl.ds(first, PADDED)
        total = taps_ref[0:1, cols] * up[pl.ds(start + HALO - 2, rows), cols]
        total = total + taps_ref[1:2, cols] * up[pl.ds(start + HALO - 1, rows), cols]
        return total + taps_ref[2:3, cols] * up[pl.ds(start + HALO, rows), cols]

    for start in range(0, LOCAL, rows):
        gate = 0.5 * conv(start, 0)
        value = pltpu.roll(conv(start, 2 * UNITS - PADDED), UNITS, 1)
        both = (gate + gate * jnp.tanh(gate)) * value
        both = jnp.where(lane < UNITS, both, 0.0)
        hidden[pl.ds(start, rows), :] = both.astype(jnp.bfloat16)
    on_copies(len(CHUNKS) - 1, lambda copy: copy.wait())
    for z in range(0, RING, 2):
        part = lax.dot_general(
            hidden[...],
            weights[z : z + 2, :, :, 0:PADDED].reshape(2 * D // RING, PADDED),
            (((1,), (1,)), ((), ())),
            preferred_element_type=jnp.float32,
        ).astype(jnp.bfloat16)
        cols = pl.ds(z * (D // RING), 2 * D // RING)
        for owner, (even, odd) in enumerate(((out_own, out_other), (out_other, out_own))):

            @pl.when(core == owner)
            def _():
                for x in range(LOCAL // OWN // 2):
                    even[x, :, cols] = part[2 * x * OWN : (2 * x + 1) * OWN]
                    odd[x, :, cols] = part[(2 * x + 1) * OWN : (2 * x + 2) * OWN]


def feed_forward(own, other, halos, taps, blocks):
    half = jax.ShapeDtypeStruct((LOCAL // OWN // 2, OWN, D), jnp.bfloat16)
    return pl.pallas_call(
        feed_forward_kernel,
        out_shape=(half, half),
        in_specs=[pl.BlockSpec(memory_space=pl.ANY)] * 4
        + [pl.BlockSpec(memory_space=pltpu.VMEM)]
        + [pl.BlockSpec(memory_space=pl.ANY)] * RING,
        out_specs=[pl.BlockSpec(memory_space=pltpu.VMEM)] * 2,
        scratch_shapes=[
            pltpu.VMEM((RING, RING, D // RING // RING, WIDE), jnp.bfloat16),
            pltpu.VMEM((HALO + LOCAL, D), jnp.bfloat16),
            pltpu.VMEM((HALO + LOCAL, 2 * UNITS), jnp.float32),
            pltpu.VMEM((LOCAL, PADDED), jnp.bfloat16),
            pltpu.SemaphoreType.DMA((len(CHUNKS), RING)),
            pltpu.SemaphoreType.DMA((LOCAL // OWN + 1,)),
        ],
        compiler_params=pltpu.CompilerParams(vmem_limit_bytes=VMEM_LIMIT),
        cost_estimate=pl.CostEstimate(
            flops=6 * LOCAL * D * UNITS,
            bytes_accessed=2 * D * WIDE + 4 * LOCAL * D,
            transcendentals=LOCAL * UNITS,
        ),
        name="feed_forward",
    )(own, other, *halos, taps, *blocks)


def device_at(z, y, x, c):
    return ((z * RING + y) * 4 + x) * 2 + c


def crossed_groups():
    groups = []
    for x in range(4):
        for fixed in range(RING):
            groups.append([device_at(fixed, k, x, 1) for k in range(RING)])
            groups.append([device_at(k, fixed, x, 0) for k in range(RING)])
    return groups


def ring_step(block, distance):
    route = []
    for z in range(RING):
        for y in range(RING):
            for x in range(4):
                route.append(
                    (device_at(z, y, x, 1), device_at((z + distance) % RING, y, x, 1))
                )
                route.append(
                    (device_at(z, y, x, 0), device_at(z, (y + distance) % RING, x, 0))
                )
    return lax.ppermute(block, ALL, route)


def halo_route(core):
    route = []
    for sp in range(RING * RING - 1):
        for x in range(4):
            route.append((device_at(0, sp, x, 1), device_at(0, sp + 1, x, core)))
    return route


def gathered_blocks(packed):
    copies = jnp.broadcast_to(packed, (RING, *packed.shape))
    own = lax.all_to_all(copies, ALL, 0, 0, tiled=True, axis_index_groups=crossed_groups())
    held = {0: own}
    for step in range(1, RING // 2 + 1):
        held[step] = ring_step(held[step - 1], 1)
        if step < RING // 2:
            held[-step] = ring_step(held[1 - step], -1)
    return [held[step] for step in STEPS]


def on_device(
    queries,
    key_states,
    value_states,
    sink_logits,
    out_weight,
    residual,
    gain_attn,
    gain_before,
    gain_after,
    gate_weight,
    value_weight,
    gate_taps,
    value_taps,
    down_weight,
):
    packed = jnp.concatenate(
        [
            jnp.pad(down_weight.T, ((0, 0), (0, PADDED - UNITS))),
            gate_weight,
            value_weight,
        ],
        axis=1,
    )
    weights = gathered_blocks(packed)
    taps = jnp.concatenate([gate_taps, value_taps], axis=1)
    other_weight = swapped(out_weight)
    own, other = attention_local(queries, key_states, value_states, sink_logits)
    other = swapped(other)
    shares = projected(own, out_weight) + projected(other, other_weight)
    attn_proj = summed_over_x(shares.astype(jnp.bfloat16))
    middle = residual.astype(jnp.float32) + rms_scale(attn_proj) * gain_attn
    normed = (rms_scale(middle) * gain_before).astype(jnp.bfloat16)
    own_rows = sent_to_all(normed, "x")
    other_rows = swapped(own_rows)
    last = own_rows[-1, OWN - HALO :]
    halos = [lax.ppermute(last, ALL, halo_route(core)) for core in range(2)]
    own, other = feed_forward(own_rows, other_rows, halos, taps, weights)
    other = swapped(other)
    pair = (own.astype(jnp.float32) + other.astype(jnp.float32)).astype(jnp.bfloat16)
    down = summed_over_x(pair)
    return (middle + rms_scale(down) * gain_after).astype(jnp.bfloat16)


def solution(mesh):
    mesh = Mesh(mesh.devices.reshape(8, 8, 4, 2), ("z", "y", "x", "c"))
    in_specs = (
        P(SP, TP),
        P(SP, TP),
        P(SP, TP),
        P(TP),
        P(TP, None),
        P((*SP, *TP), None),
        P(),
        P(),
        P(),
        P(SP, TP),
        P(SP, TP),
        P(None, TP),
        P(None, TP),
        P(TP, SP),
    )
    out_specs = P((*SP, *TP), None)
    return jax.shard_map(
        on_device, mesh=mesh, in_specs=in_specs, out_specs=out_specs, check_vma=False
    )
```

```python
import functools

import jax
import jax.numpy as jnp
from jax import lax
from jax.experimental import pallas as pl
from jax.experimental.pallas import tpu as pltpu
from jax.sharding import Mesh
from jax.sharding import PartitionSpec as P

HD = 64
WINDOW = 128
D = 2048
UNITS = 704
PADDED = 768
UP_AT = PADDED
WIDE = PADDED + 2 * UNITS
HALO = 16
LOCAL = 512
OWN = 64
SP = ("z", "y")
TP = ("x", "c")

NEG_FILL = -1e30
ALL = (*SP, *TP)
RING = 8
STEPS = (0, 1, -1, 2, -2, 3, -3, 4)
VMEM_LIMIT = 44 * 1024 * 1024


def passed_along(block, axis, distance):
    devices = range(lax.axis_size(axis))
    route = [(i - distance, i) for i in devices if i - distance in devices]
    return lax.ppermute(block, axis, route)


def swapped(block):
    return lax.ppermute(block, "c", [(0, 1), (1, 0)])


def projected(rows, weight):
    return jnp.einsum("xrk,kd->xrd", rows, weight, preferred_element_type=jnp.float32)


def summed_over_x(shares):
    return jnp.sum(lax.all_to_all(shares, "x", 0, 0, tiled=True).astype(jnp.float32), axis=0)


def sent_to_all(shard, axis):
    copies = jnp.broadcast_to(shard, (lax.axis_size(axis), *shard.shape))
    return lax.all_to_all(copies, axis, split_axis=0, concat_axis=0, tiled=True)


def rms_scale(matrix):
    return matrix * lax.rsqrt(jnp.mean(matrix * matrix, axis=-1, keepdims=True) + 1e-06)


def attention_kernel(q_ref, k_ref, v_ref, edge_ref, sink_ref, own_ref, other_ref):
    core = lax.axis_index("c")
    first = lax.axis_index("z") + lax.axis_index("y") == 0
    row = lax.broadcasted_iota(jnp.int32, (WINDOW, 2 * WINDOW), 0)
    key = lax.broadcasted_iota(jnp.int32, (WINDOW, 2 * WINDOW), 1)
    inside = (key > row) & (key <= row + WINDOW)
    none = jnp.zeros((HD, 2 * WINDOW), jnp.bfloat16)
    for n in range(LOCAL // WINDOW):
        if n == 0:
            keys = jnp.concatenate([edge_ref[:HD], k_ref[:, :WINDOW]], axis=1)
            values = jnp.concatenate([edge_ref[HD:], v_ref[:, :WINDOW]], axis=1)
            seen = inside & ((key >= WINDOW) | jnp.logical_not(first))
        else:
            cols = pl.ds((n - 1) * WINDOW, 2 * WINDOW)
            keys, values, seen = k_ref[:, cols], v_ref[:, cols], inside
        for pair in range(2):
            cols = pl.ds(pair * 2 * HD, 2 * HD)
            query = q_ref[pl.ds(n * WINDOW, WINDOW), cols]
            result = jnp.zeros((WINDOW, 2 * HD), jnp.float32)
            for odd in range(2):
                placed = lambda part: jnp.concatenate([none, part] if odd else [part, none], axis=0)
                scores = jnp.dot(query, placed(keys), preferred_element_type=jnp.float32)
                scores = jnp.where(seen, scores * HD ** (-0.5), NEG_FILL)
                sink = sink_ref[2 * pair + odd]
                top = jnp.maximum(jnp.max(scores, axis=-1, keepdims=True), sink)
                expo = jnp.exp(scores - top)
                total = jnp.sum(expo, axis=-1, keepdims=True) + jnp.exp(sink - top)
                probs = (expo / total).astype(jnp.bfloat16)
                result = result + lax.dot_general(
                    probs,
                    placed(values),
                    (((1,), (1,)), ((), ())),
                    preferred_element_type=jnp.float32,
                )
            result = result.astype(jnp.bfloat16)

            @pl.when(core == 0)
            def _():
                own_ref[n, :, cols] = result[:OWN]
                other_ref[n, :, cols] = result[OWN:]

            @pl.when(core == 1)
            def _():
                own_ref[n, :, cols] = result[OWN:]
                other_ref[n, :, cols] = result[:OWN]


def attention_local(queries, key_states, value_states, sink_logits):
    keys, values = key_states.T, value_states.T
    edge = jnp.concatenate([keys[:, LOCAL - WINDOW :], values[:, LOCAL - WINDOW :]], axis=0)
    edge = passed_along(edge, SP, 1)
    half = jax.ShapeDtypeStruct((LOCAL // OWN // 2, OWN, 4 * HD), jnp.bfloat16)
    vmem = pl.BlockSpec(memory_space=pltpu.VMEM)
    return pl.pallas_call(
        attention_kernel,
        out_shape=(half, half),
        in_specs=[vmem] * 4 + [pl.BlockSpec(memory_space=pltpu.SMEM)],
        out_specs=(vmem, vmem),
        compiler_params=pltpu.CompilerParams(vmem_limit_bytes=16 * 1024 * 1024),
        cost_estimate=pl.CostEstimate(
            flops=8 * 4 * LOCAL * 2 * WINDOW * HD,
            bytes_accessed=8 * LOCAL * 4 * HD,
            transcendentals=4 * LOCAL * 2 * WINDOW,
        ),
        name="attention",
    )(queries, keys, values, edge, sink_logits)


def feed_forward_kernel(own_ref, other_ref, halo_0, halo_1, taps_ref, *refs):
    blocks = refs[:RING]
    out_own, out_other, weights, x_ref, up, hidden, sems, row_sems = refs[RING:]
    core = lax.axis_index("c")
    place = jnp.where(core == 1, lax.axis_index("z"), lax.axis_index("y"))

    def on_copies(act):
        for k, (block, step) in enumerate(zip(blocks, STEPS)):
            source = lax.rem(place - step + RING, RING)
            sem = sems.at[k]

            @pl.when(core == 1)
            def _():
                act(pltpu.make_async_copy(block, weights.at[source], sem))

            @pl.when(core == 0)
            def _():
                act(pltpu.make_async_copy(block, weights.at[:, source], sem))

    def on_rows(act):
        for x in range(LOCAL // OWN // 2):
            for k, (part, at) in enumerate(((own_ref, core), (other_ref, 1 - core))):
                start = pl.multiple_of(HALO + OWN * (2 * x + at), HALO)
                act(
                    pltpu.make_async_copy(
                        part.at[x], x_ref.at[pl.ds(start, OWN)], row_sems.at[2 * x + k]
                    )
                )
        for k, halo in enumerate((halo_0, halo_1)):

            @pl.when(core == k)
            def _():
                act(pltpu.make_async_copy(halo, x_ref.at[pl.ds(0, HALO)], row_sems.at[8]))

    on_rows(lambda copy: copy.start())
    on_copies(lambda copy: copy.start())
    on_rows(lambda copy: copy.wait())
    on_copies(lambda copy: copy.wait())
    for at in range(0, 2 * UNITS, 256):
        width = min(256, 2 * UNITS - at)
        part = jnp.dot(
            x_ref[...],
            weights[:, :, :, UP_AT + at : UP_AT + at + width].reshape(D, width),
            preferred_element_type=jnp.float32,
        )
        up[:, at : at + width] = part.astype(jnp.bfloat16).astype(jnp.float32)
    rows = 64
    lane = lax.broadcasted_iota(jnp.int32, (rows, PADDED), 1)

    def conv(start, first):
        cols = pl.ds(first, PADDED)
        total = taps_ref[0:1, cols] * up[pl.ds(start + HALO - 2, rows), cols]
        total = total + taps_ref[1:2, cols] * up[pl.ds(start + HALO - 1, rows), cols]
        return total + taps_ref[2:3, cols] * up[pl.ds(start + HALO, rows), cols]

    for start in range(0, LOCAL, rows):
        gate = 0.5 * conv(start, 0)
        value = pltpu.roll(conv(start, 2 * UNITS - PADDED), UNITS, 1)
        both = (gate + gate * jnp.tanh(gate)) * value
        both = jnp.where(lane < UNITS, both, 0.0)
        hidden[pl.ds(start, rows), :] = both.astype(jnp.bfloat16)
    for z in range(0, RING, 2):
        part = lax.dot_general(
            hidden[...],
            weights[z : z + 2, :, :, 0:PADDED].reshape(2 * D // RING, PADDED),
            (((1,), (1,)), ((), ())),
            preferred_element_type=jnp.float32,
        ).astype(jnp.bfloat16)
        cols = pl.ds(z * (D // RING), 2 * D // RING)
        for owner, (even, odd) in enumerate(((out_own, out_other), (out_other, out_own))):

            @pl.when(core == owner)
            def _():
                for x in range(LOCAL // OWN // 2):
                    even[x, :, cols] = part[2 * x * OWN : (2 * x + 1) * OWN]
                    odd[x, :, cols] = part[(2 * x + 1) * OWN : (2 * x + 2) * OWN]


def feed_forward(own, other, halos, taps, blocks):
    half = jax.ShapeDtypeStruct((LOCAL // OWN // 2, OWN, D), jnp.bfloat16)
    return pl.pallas_call(
        feed_forward_kernel,
        out_shape=(half, half),
        in_specs=[pl.BlockSpec(memory_space=pl.ANY)] * 4
        + [pl.BlockSpec(memory_space=pltpu.VMEM)]
        + [pl.BlockSpec(memory_space=pl.ANY)] * RING,
        out_specs=[pl.BlockSpec(memory_space=pltpu.VMEM)] * 2,
        scratch_shapes=[
            pltpu.VMEM((RING, RING, D // RING // RING, WIDE), jnp.bfloat16),
            pltpu.VMEM((HALO + LOCAL, D), jnp.bfloat16),
            pltpu.VMEM((HALO + LOCAL, 2 * UNITS), jnp.float32),
            pltpu.VMEM((LOCAL, PADDED), jnp.bfloat16),
            pltpu.SemaphoreType.DMA((RING,)),
            pltpu.SemaphoreType.DMA((LOCAL // OWN + 1,)),
        ],
        compiler_params=pltpu.CompilerParams(vmem_limit_bytes=VMEM_LIMIT),
        cost_estimate=pl.CostEstimate(
            flops=6 * LOCAL * D * UNITS,
            bytes_accessed=2 * D * WIDE + 4 * LOCAL * D,
            transcendentals=LOCAL * UNITS,
        ),
        name="feed_forward",
    )(own, other, *halos, taps, *blocks)


def device_at(z, y, x, c):
    return ((z * RING + y) * 4 + x) * 2 + c


def crossed_groups():
    groups = []
    for x in range(4):
        for fixed in range(RING):
            groups.append([device_at(fixed, k, x, 1) for k in range(RING)])
            groups.append([device_at(k, fixed, x, 0) for k in range(RING)])
    return groups


def ring_step(block, distance):
    route = []
    for z in range(RING):
        for y in range(RING):
            for x in range(4):
                route.append(
                    (device_at(z, y, x, 1), device_at((z + distance) % RING, y, x, 1))
                )
                route.append(
                    (device_at(z, y, x, 0), device_at(z, (y + distance) % RING, x, 0))
                )
    return lax.ppermute(block, ALL, route)


def halo_route(core):
    route = []
    for sp in range(RING * RING - 1):
        for x in range(4):
            route.append((device_at(0, sp, x, 1), device_at(0, sp + 1, x, core)))
    return route


def gathered_blocks(copies):
    own = lax.all_to_all(copies, ALL, 0, 0, tiled=True, axis_index_groups=crossed_groups())
    held = {0: own}
    for step in range(1, RING // 2 + 1):
        held[step] = ring_step(held[step - 1], 1)
        if step < RING // 2:
            held[-step] = ring_step(held[1 - step], -1)
    return [held[step] for step in STEPS]


def pack_kernel(down_hbm, gate_hbm, value_hbm, out_ref, down, gate, value, sems):
    pairs = ((down_hbm, down), (gate_hbm, gate), (value_hbm, value))
    copies = [
        pltpu.make_async_copy(source, target, sems.at[k]) for k, (source, target) in enumerate(pairs)
    ]
    for copy in copies:
        copy.start()
    for copy in copies:
        copy.wait()
    for k in range(RING):
        out_ref[k, :, :UNITS] = down[...]
        out_ref[k, :, UNITS:PADDED] = jnp.zeros((OWN // 2, PADDED - UNITS), jnp.bfloat16)
        out_ref[k, :, PADDED : PADDED + UNITS] = gate[...]
        out_ref[k, :, PADDED + UNITS :] = value[...]


def packed_copies(down_weight, gate_weight, value_weight):
    part = pltpu.VMEM((OWN // 2, UNITS), jnp.bfloat16)
    return pl.pallas_call(
        pack_kernel,
        out_shape=jax.ShapeDtypeStruct((RING, OWN // 2, WIDE), jnp.bfloat16),
        in_specs=[pl.BlockSpec(memory_space=pl.ANY)] * 3,
        out_specs=pl.BlockSpec(memory_space=pltpu.VMEM),
        scratch_shapes=[part, part, part, pltpu.SemaphoreType.DMA((3,))],
        compiler_params=pltpu.CompilerParams(vmem_limit_bytes=60 * 1024 * 1024),
        cost_estimate=pl.CostEstimate(
            flops=0, bytes_accessed=2 * RING * OWN // 2 * WIDE, transcendentals=0
        ),
        name="pack",
    )(down_weight.T, gate_weight, value_weight)


def on_device(
    queries,
    key_states,
    value_states,
    sink_logits,
    out_weight,
    residual,
    gain_attn,
    gain_before,
    gain_after,
    gate_weight,
    value_weight,
    gate_taps,
    value_taps,
    down_weight,
):
    copies = packed_copies(down_weight, gate_weight, value_weight)
    copies, out_weight, key_states = lax.optimization_barrier((copies, out_weight, key_states))
    weights = gathered_blocks(copies)
    taps = jnp.concatenate([gate_taps, value_taps], axis=1)
    other_weight = swapped(out_weight)
    own, other = attention_local(queries, key_states, value_states, sink_logits)
    other = swapped(other)
    shares = projected(own, out_weight) + projected(other, other_weight)
    attn_proj = summed_over_x(shares.astype(jnp.bfloat16))
    middle = residual.astype(jnp.float32) + rms_scale(attn_proj) * gain_attn
    normed = (rms_scale(middle) * gain_before).astype(jnp.bfloat16)
    own_rows = sent_to_all(normed, "x")
    other_rows = swapped(own_rows)
    last = own_rows[-1, OWN - HALO :]
    halos = [lax.ppermute(last, ALL, halo_route(core)) for core in range(2)]
    own, other = feed_forward(own_rows, other_rows, halos, taps, weights)
    other = swapped(other)
    pair = (own.astype(jnp.float32) + other.astype(jnp.float32)).astype(jnp.bfloat16)
    down = summed_over_x(pair)
    return (middle + rms_scale(down) * gain_after).astype(jnp.bfloat16)


def solution(mesh):
    mesh = Mesh(mesh.devices.reshape(8, 8, 4, 2), ("z", "y", "x", "c"))
    in_specs = (
        P(SP, TP),
        P(SP, TP),
        P(SP, TP),
        P(TP),
        P(TP, None),
        P((*SP, *TP), None),
        P(),
        P(),
        P(),
        P(SP, TP),
        P(SP, TP),
        P(None, TP),
        P(None, TP),
        P(TP, SP),
    )
    out_specs = P((*SP, *TP), None)
    return jax.shard_map(
        on_device, mesh=mesh, in_specs=in_specs, out_specs=out_specs, check_vma=False
    )
```

```python
import functools

import jax
import jax.numpy as jnp
from jax import lax
from jax.experimental import pallas as pl
from jax.experimental.pallas import tpu as pltpu
from jax.sharding import Mesh
from jax.sharding import PartitionSpec as P

HD = 64
WINDOW = 128
D = 2048
UNITS = 704
PADDED = 768
UP_AT = PADDED
WIDE = PADDED + 2 * UNITS
HALO = 16
LOCAL = 512
OWN = 64
SP = ("z", "y")
TP = ("x", "c")

NEG_FILL = -1e30
ALL = (*SP, *TP)
RING = 8
STEPS = (0, 1, -1, 2, -2, 3, -3, 4)
CHUNKS = ((UP_AT, 2 * UNITS), (0, PADDED))
VMEM_LIMIT = 44 * 1024 * 1024


def passed_along(block, axis, distance):
    devices = range(lax.axis_size(axis))
    route = [(i - distance, i) for i in devices if i - distance in devices]
    return lax.ppermute(block, axis, route)


def swapped(block):
    return lax.ppermute(block, "c", [(0, 1), (1, 0)])


def projected(rows, weight):
    return jnp.einsum("xrk,kd->xrd", rows, weight, preferred_element_type=jnp.float32)


def summed_over_x(shares):
    return jnp.sum(lax.all_to_all(shares, "x", 0, 0, tiled=True).astype(jnp.float32), axis=0)


def sent_to_all(shard, axis):
    copies = jnp.broadcast_to(shard, (lax.axis_size(axis), *shard.shape))
    return lax.all_to_all(copies, axis, split_axis=0, concat_axis=0, tiled=True)


def rms_scale(matrix):
    return matrix * lax.rsqrt(jnp.mean(matrix * matrix, axis=-1, keepdims=True) + 1e-06)


def attention_kernel(q_ref, k_ref, v_ref, edge_ref, sink_ref, own_ref, other_ref):
    core = lax.axis_index("c")
    first = lax.axis_index("z") + lax.axis_index("y") == 0
    row = lax.broadcasted_iota(jnp.int32, (WINDOW, 2 * WINDOW), 0)
    key = lax.broadcasted_iota(jnp.int32, (WINDOW, 2 * WINDOW), 1)
    inside = (key > row) & (key <= row + WINDOW)
    none = jnp.zeros((HD, 2 * WINDOW), jnp.bfloat16)
    for n in range(LOCAL // WINDOW):
        if n == 0:
            keys = jnp.concatenate([edge_ref[:HD], k_ref[:, :WINDOW]], axis=1)
            values = jnp.concatenate([edge_ref[HD:], v_ref[:, :WINDOW]], axis=1)
            seen = inside & ((key >= WINDOW) | jnp.logical_not(first))
        else:
            cols = pl.ds((n - 1) * WINDOW, 2 * WINDOW)
            keys, values, seen = k_ref[:, cols], v_ref[:, cols], inside
        for pair in range(2):
            cols = pl.ds(pair * 2 * HD, 2 * HD)
            query = q_ref[pl.ds(n * WINDOW, WINDOW), cols]
            result = jnp.zeros((WINDOW, 2 * HD), jnp.float32)
            for odd in range(2):
                placed = lambda part: jnp.concatenate([none, part] if odd else [part, none], axis=0)
                scores = jnp.dot(query, placed(keys), preferred_element_type=jnp.float32)
                scores = jnp.where(seen, scores * HD ** (-0.5), NEG_FILL)
                sink = sink_ref[2 * pair + odd]
                top = jnp.maximum(jnp.max(scores, axis=-1, keepdims=True), sink)
                expo = jnp.exp(scores - top)
                total = jnp.sum(expo, axis=-1, keepdims=True) + jnp.exp(sink - top)
                probs = (expo / total).astype(jnp.bfloat16)
                result = result + lax.dot_general(
                    probs,
                    placed(values),
                    (((1,), (1,)), ((), ())),
                    preferred_element_type=jnp.float32,
                )
            result = result.astype(jnp.bfloat16)

            @pl.when(core == 0)
            def _():
                own_ref[n, :, cols] = result[:OWN]
                other_ref[n, :, cols] = result[OWN:]

            @pl.when(core == 1)
            def _():
                own_ref[n, :, cols] = result[OWN:]
                other_ref[n, :, cols] = result[:OWN]


def attention_local(queries, key_states, value_states, sink_logits):
    keys, values = key_states.T, value_states.T
    edge = jnp.concatenate([keys[:, LOCAL - WINDOW :], values[:, LOCAL - WINDOW :]], axis=0)
    edge = passed_along(edge, SP, 1)
    half = jax.ShapeDtypeStruct((LOCAL // OWN // 2, OWN, 4 * HD), jnp.bfloat16)
    vmem = pl.BlockSpec(memory_space=pltpu.VMEM)
    return pl.pallas_call(
        attention_kernel,
        out_shape=(half, half),
        in_specs=[vmem] * 4 + [pl.BlockSpec(memory_space=pltpu.SMEM)],
        out_specs=(vmem, vmem),
        compiler_params=pltpu.CompilerParams(vmem_limit_bytes=16 * 1024 * 1024),
        cost_estimate=pl.CostEstimate(
            flops=8 * 4 * LOCAL * 2 * WINDOW * HD,
            bytes_accessed=8 * LOCAL * 4 * HD,
            transcendentals=4 * LOCAL * 2 * WINDOW,
        ),
        name="attention",
    )(queries, keys, values, edge, sink_logits)


def feed_forward_kernel(own_ref, other_ref, halo_0, halo_1, taps_ref, *refs):
    blocks = refs[:RING]
    out_own, out_other, weights, x_ref, up, hidden, sems, row_sems = refs[RING:]
    core = lax.axis_index("c")
    place = jnp.where(core == 1, lax.axis_index("z"), lax.axis_index("y"))

    def on_copies(chunk, act):
        cols = pl.ds(*CHUNKS[chunk])
        for k, (block, step) in enumerate(zip(blocks, STEPS)):
            source = lax.rem(place - step + RING, RING)
            sem = sems.at[chunk, k]

            @pl.when(core == 1)
            def _():
                act(
                    pltpu.make_async_copy(
                        block.at[:, :, cols], weights.at[source, :, :, cols], sem
                    )
                )

            @pl.when(core == 0)
            def _():
                act(
                    pltpu.make_async_copy(
                        block.at[:, :, cols], weights.at[:, source, :, cols], sem
                    )
                )

    def on_rows(act):
        for x in range(LOCAL // OWN // 2):
            for k, (part, at) in enumerate(((own_ref, core), (other_ref, 1 - core))):
                start = pl.multiple_of(HALO + OWN * (2 * x + at), HALO)
                act(
                    pltpu.make_async_copy(
                        part.at[x], x_ref.at[pl.ds(start, OWN)], row_sems.at[2 * x + k]
                    )
                )
        for k, halo in enumerate((halo_0, halo_1)):

            @pl.when(core == k)
            def _():
                act(pltpu.make_async_copy(halo, x_ref.at[pl.ds(0, HALO)], row_sems.at[8]))

    on_rows(lambda copy: copy.start())
    for chunk in range(len(CHUNKS)):
        on_copies(chunk, lambda copy: copy.start())
    on_rows(lambda copy: copy.wait())
    for chunk, (at, width) in enumerate(CHUNKS[:-1]):
        on_copies(chunk, lambda copy: copy.wait())
        for sub in range(at, at + width, 256):
            wide = min(256, at + width - sub)
            part = jnp.dot(
                x_ref[...],
                weights[:, :, :, sub : sub + wide].reshape(D, wide),
                preferred_element_type=jnp.float32,
            )
            up[:, sub - UP_AT : sub - UP_AT + wide] = part.astype(jnp.bfloat16).astype(
                jnp.float32
            )
    rows = 64
    lane = lax.broadcasted_iota(jnp.int32, (rows, PADDED), 1)

    def conv(start, first):
        cols = pl.ds(first, PADDED)
        total = taps_ref[0:1, cols] * up[pl.ds(start + HALO - 2, rows), cols]
        total = total + taps_ref[1:2, cols] * up[pl.ds(start + HALO - 1, rows), cols]
        return total + taps_ref[2:3, cols] * up[pl.ds(start + HALO, rows), cols]

    for start in range(0, LOCAL, rows):
        gate = 0.5 * conv(start, 0)
        value = pltpu.roll(conv(start, 2 * UNITS - PADDED), UNITS, 1)
        both = (gate + gate * jnp.tanh(gate)) * value
        both = jnp.where(lane < UNITS, both, 0.0)
        hidden[pl.ds(start, rows), :] = both.astype(jnp.bfloat16)
    on_copies(len(CHUNKS) - 1, lambda copy: copy.wait())
    for z in range(0, RING, 2):
        part = lax.dot_general(
            hidden[...],
            weights[z : z + 2, :, :, 0:PADDED].reshape(2 * D // RING, PADDED),
            (((1,), (1,)), ((), ())),
            preferred_element_type=jnp.float32,
        ).astype(jnp.bfloat16)
        cols = pl.ds(z * (D // RING), 2 * D // RING)
        for owner, (even, odd) in enumerate(((out_own, out_other), (out_other, out_own))):

            @pl.when(core == owner)
            def _():
                for x in range(LOCAL // OWN // 2):
                    even[x, :, cols] = part[2 * x * OWN : (2 * x + 1) * OWN]
                    odd[x, :, cols] = part[(2 * x + 1) * OWN : (2 * x + 2) * OWN]


def feed_forward(own, other, halos, taps, blocks):
    half = jax.ShapeDtypeStruct((LOCAL // OWN // 2, OWN, D), jnp.bfloat16)
    return pl.pallas_call(
        feed_forward_kernel,
        out_shape=(half, half),
        in_specs=[pl.BlockSpec(memory_space=pl.ANY)] * 4
        + [pl.BlockSpec(memory_space=pltpu.VMEM)]
        + [pl.BlockSpec(memory_space=pl.ANY)] * RING,
        out_specs=[pl.BlockSpec(memory_space=pltpu.VMEM)] * 2,
        scratch_shapes=[
            pltpu.VMEM((RING, RING, D // RING // RING, WIDE), jnp.bfloat16),
            pltpu.VMEM((HALO + LOCAL, D), jnp.bfloat16),
            pltpu.VMEM((HALO + LOCAL, 2 * UNITS), jnp.float32),
            pltpu.VMEM((LOCAL, PADDED), jnp.bfloat16),
            pltpu.SemaphoreType.DMA((len(CHUNKS), RING)),
            pltpu.SemaphoreType.DMA((LOCAL // OWN + 1,)),
        ],
        compiler_params=pltpu.CompilerParams(vmem_limit_bytes=VMEM_LIMIT),
        cost_estimate=pl.CostEstimate(
            flops=6 * LOCAL * D * UNITS,
            bytes_accessed=2 * D * WIDE + 4 * LOCAL * D,
            transcendentals=LOCAL * UNITS,
        ),
        name="feed_forward",
    )(own, other, *halos, taps, *blocks)


def device_at(z, y, x, c):
    return ((z * RING + y) * 4 + x) * 2 + c


def crossed_groups():
    groups = []
    for x in range(4):
        for fixed in range(RING):
            groups.append([device_at(fixed, k, x, 1) for k in range(RING)])
            groups.append([device_at(k, fixed, x, 0) for k in range(RING)])
    return groups


def ring_step(block, distance):
    route = []
    for z in range(RING):
        for y in range(RING):
            for x in range(4):
                route.append(
                    (device_at(z, y, x, 1), device_at((z + distance) % RING, y, x, 1))
                )
                route.append(
                    (device_at(z, y, x, 0), device_at(z, (y + distance) % RING, x, 0))
                )
    return lax.ppermute(block, ALL, route)


def halo_route(core):
    route = []
    for sp in range(RING * RING - 1):
        for x in range(4):
            route.append((device_at(0, sp, x, 1), device_at(0, sp + 1, x, core)))
    return route


def gathered_blocks(copies):
    own = lax.all_to_all(copies, ALL, 0, 0, tiled=True, axis_index_groups=crossed_groups())
    held = {0: own}
    for step in range(1, RING // 2 + 1):
        held[step] = ring_step(held[step - 1], 1)
        if step < RING // 2:
            held[-step] = ring_step(held[1 - step], -1)
    return [held[step] for step in STEPS]


def pack_kernel(down_hbm, gate_hbm, value_hbm, out_ref, down, gate, value, sems):
    pairs = ((down_hbm, down), (gate_hbm, gate), (value_hbm, value))
    copies = [
        pltpu.make_async_copy(source, target, sems.at[k]) for k, (source, target) in enumerate(pairs)
    ]
    for copy in copies:
        copy.start()
    for copy in copies:
        copy.wait()
    for k in range(RING):
        out_ref[k, :, :UNITS] = down[...]
        out_ref[k, :, UNITS:PADDED] = jnp.zeros((OWN // 2, PADDED - UNITS), jnp.bfloat16)
        out_ref[k, :, PADDED : PADDED + UNITS] = gate[...]
        out_ref[k, :, PADDED + UNITS :] = value[...]


def packed_copies(down_weight, gate_weight, value_weight):
    part = pltpu.VMEM((OWN // 2, UNITS), jnp.bfloat16)
    return pl.pallas_call(
        pack_kernel,
        out_shape=jax.ShapeDtypeStruct((RING, OWN // 2, WIDE), jnp.bfloat16),
        in_specs=[pl.BlockSpec(memory_space=pl.ANY)] * 3,
        out_specs=pl.BlockSpec(memory_space=pltpu.VMEM),
        scratch_shapes=[part, part, part, pltpu.SemaphoreType.DMA((3,))],
        compiler_params=pltpu.CompilerParams(vmem_limit_bytes=60 * 1024 * 1024),
        cost_estimate=pl.CostEstimate(
            flops=0, bytes_accessed=2 * RING * OWN // 2 * WIDE, transcendentals=0
        ),
        name="pack",
    )(down_weight.T, gate_weight, value_weight)


def on_device(
    queries,
    key_states,
    value_states,
    sink_logits,
    out_weight,
    residual,
    gain_attn,
    gain_before,
    gain_after,
    gate_weight,
    value_weight,
    gate_taps,
    value_taps,
    down_weight,
):
    copies = packed_copies(down_weight, gate_weight, value_weight)
    copies, out_weight, key_states = lax.optimization_barrier((copies, out_weight, key_states))
    weights = gathered_blocks(copies)
    taps = jnp.concatenate([gate_taps, value_taps], axis=1)
    other_weight = swapped(out_weight)
    own, other = attention_local(queries, key_states, value_states, sink_logits)
    other = swapped(other)
    shares = projected(own, out_weight) + projected(other, other_weight)
    attn_proj = summed_over_x(shares.astype(jnp.bfloat16))
    middle = residual.astype(jnp.float32) + rms_scale(attn_proj) * gain_attn
    normed = (rms_scale(middle) * gain_before).astype(jnp.bfloat16)
    own_rows = sent_to_all(normed, "x")
    other_rows = swapped(own_rows)
    last = own_rows[-1, OWN - HALO :]
    halos = [lax.ppermute(last, ALL, halo_route(core)) for core in range(2)]
    own, other = feed_forward(own_rows, other_rows, halos, taps, weights)
    other = swapped(other)
    pair = (own.astype(jnp.float32) + other.astype(jnp.float32)).astype(jnp.bfloat16)
    down = summed_over_x(pair)
    return (middle + rms_scale(down) * gain_after).astype(jnp.bfloat16)


def solution(mesh):
    mesh = Mesh(mesh.devices.reshape(8, 8, 4, 2), ("z", "y", "x", "c"))
    in_specs = (
        P(SP, TP),
        P(SP, TP),
        P(SP, TP),
        P(TP),
        P(TP, None),
        P((*SP, *TP), None),
        P(),
        P(),
        P(),
        P(SP, TP),
        P(SP, TP),
        P(None, TP),
        P(None, TP),
        P(TP, SP),
    )
    out_specs = P((*SP, *TP), None)
    return jax.shard_map(
        on_device, mesh=mesh, in_specs=in_specs, out_specs=out_specs, check_vma=False
    )
```
